1024 devices in a mesh: ep: 64 (over z, y), tp: 16 (over x, core).
Axes of the slice: x: 8, y: 8, z: 8, core: 2. Of those that a mesh axis runs over, the one named last changes fastest.
Arguments:
- tokens: bfloat16 [8192, 2048], P('ep'), may hold values from -36 to 36, as said below
- norm_gain: float32 [2048], replicated, may hold values from 0.1 to 1.9
- chosen: int32 [8, 2048], replicated, may hold values from 0 to 8191, as said below
- slot_weight: float32 [8, 2048], replicated, may hold values from 0.1 to 1
- gate_weight: bfloat16 [8, 2048, 4096], P(None, 'ep', 'tp'), may hold values from -0.125 to 0.125
- up_weight: bfloat16 [8, 2048, 4096], P(None, 'ep', 'tp'), may hold values from -0.125 to 0.125
- down_weight: bfloat16 [8, 2048, 4096], P(None, 'ep', 'tp'), may hold values from -0.09375 to 0.09375
Outputs:
- mixed: bfloat16 [8192, 2048], P('ep', 'tp')
The draws below stay inside these ranges and needn't reach their ends.
Inputs may be any that keep to these rules, and one draw needn't show every extreme that they name: `tokens`: each entry is the scaled entry of a bounded draw; rows and features differ in scale. `chosen`: the 2048 slots of an expert name distinct tokens. Slots of an expert fall into aligned blocks of 256; within a block the token numbers ascend, and at most 8 of them lie among the 128 tokens of one index of ep (tokens i * 128 onward belong to index i); in every block some index supplies exactly 8.
All inputs are finite; a program needn't handle non-finite values.
Results may differ from the reference program's by a relative error of at most 0.019.
Values may be sent and summed in bfloat16 or wider, within the bound.
A program may use at most 32 MiB of HBM per device.

```python
import math
import jax
import jax.numpy as jnp
from jax import lax

D = 2048
FF = 4096
EXPERTS = 8
TOK_DEV = 128
TOKENS = 8192
CAP = 2048
SLOTS_DEV = 256
SLOT_CAP = 8
N_TP = 16


def draw_tokens(key, part):
    row_key, column_key, base_key = jax.random.split(jax.random.fold_in(key, 3), 3)
    row_scale = jnp.exp(jax.random.uniform(row_key, (TOKENS, 1), jnp.float32, math.log(0.3), math.log(3.0)))
    column_scale = jnp.exp(jax.random.uniform(column_key, (1, D), jnp.float32, math.log(0.3), math.log(3.0)))
    base = jax.random.normal(base_key, (TOKENS, D), jnp.float32)
    base = jnp.clip(base, -4.0, 4.0)
    return (base * row_scale * column_scale).astype(jnp.bfloat16)


def draw_chosen(key, part):
    owners_total = TOKENS // TOK_DEV
    group_size = owners_total // EXPERTS
    seats_total = owners_total * SLOT_CAP
    order_key, seat_key, forced_key = jax.random.split(jax.random.fold_in(key, 17), 3)
    order_scores = jax.random.randint(order_key, (EXPERTS, owners_total, TOK_DEV), 0, 1 << 20) * TOK_DEV
    order_scores = order_scores + jnp.arange(TOK_DEV, dtype=jnp.int32)
    token_order = jnp.argsort(order_scores, axis=-1).astype(jnp.int32)
    seat_scores = jax.random.randint(seat_key, (owners_total, seats_total), 0, 1 << 20) * seats_total
    seat_scores = seat_scores + jnp.arange(seats_total, dtype=jnp.int32)
    forced_owner = jax.random.randint(forced_key, (owners_total, 1), 0, owners_total)
    seat_owner_all = jnp.arange(seats_total, dtype=jnp.int32) // SLOT_CAP
    seat_scores = jnp.where(seat_owner_all[None, :] == forced_owner, seat_scores - (1 << 30), seat_scores)
    picked_seats = jnp.argsort(seat_scores, axis=-1)[:, :SLOTS_DEV].astype(jnp.int32)
    seat_owner = picked_seats // SLOT_CAP
    seat_rank = picked_seats % SLOT_CAP
    piece_index = jnp.arange(owners_total, dtype=jnp.int32)[:, None]
    expert_index = piece_index // group_size
    within = piece_index % group_size * SLOT_CAP + seat_rank
    local_token = token_order[expert_index, seat_owner, within]
    global_token = seat_owner * TOK_DEV + local_token
    return jnp.sort(global_token, axis=-1).reshape(EXPERTS, CAP).astype(jnp.int32)


def steps_of(rng, dims, cuts, least, largest):
    def one(position, shards_of):
        heights = jax.random.uniform(jax.random.fold_in(jax.random.fold_in(rng, 6), position), (shards_of,), jnp.float32, least / len(cuts), largest / len(cuts))
        return jnp.repeat(jnp.exp(heights), dims[position] // shards_of).reshape((-1,) + (1,) * (len(dims) - position - 1))

    factor_of = one(*cuts[0])
    for cut in cuts[1:]:
        factor_of = factor_of * one(*cut)
    return factor_of


def noise(key, dims, deviation, reach, shards=(), kind=jnp.bfloat16):
    values = jax.random.normal(key, dims, jnp.float32) * deviation
    if len(shards) > 0:
        values = steps_of(key, dims, shards, -0.22, 0.18) * values
    return jnp.clip(values, min=-reach, max=reach).astype(kind)


def setup_inputs(seed: int = 0) -> dict:
    key_of = jax.random.split(jax.random.key(seed), 8)
    return {
        "tokens": draw_tokens(jax.random.fold_in(key_of[7], 71), 0),
        "norm_gain": jnp.clip(1.0 + 0.18 * jax.random.normal(key_of[1], (D,), jnp.float32), 0.1, 1.9),
        "chosen": draw_chosen(jax.random.fold_in(key_of[7], 71), 0),
        "slot_weight": jnp.clip(jnp.exp(jax.random.uniform(key_of[3], (EXPERTS, CAP), jnp.float32, math.log(0.1), math.log(1.0))), 0.1, 1.0),
        "gate_weight": noise(key_of[4], (EXPERTS, D, FF), D ** -0.5, 0.125, ((1, 64), (2, 16))),
        "up_weight": noise(key_of[5], (EXPERTS, D, FF), D ** -0.5, 0.125, ((1, 64), (2, 16))),
        "down_weight": noise(key_of[6], (EXPERTS, D, FF), FF ** -0.5, 0.09375, ((1, 64), (2, 16))),
    }


EPSILON = 1e-06

def reference(tokens, norm_gain, chosen, slot_weight, gate_weight, up_weight, down_weight):
    values = tokens.astype(jnp.float32)
    scaled = values * lax.rsqrt(lax.optimization_barrier(jnp.mean(values * values, axis=1, keepdims=True)) + EPSILON)
    normed = (scaled * norm_gain).astype(jnp.bfloat16)
    block_units = FF // N_TP

    def per_expert(accumulated, operands):
        picked, weights, gate_w, up_w, down_w = operands
        gathered = jnp.take(normed, picked, axis=0)
        gate_part = jnp.dot(gathered, gate_w, preferred_element_type=jnp.float32)
        up_part = jnp.dot(gathered, up_w, preferred_element_type=jnp.float32)
        hidden = (jax.nn.silu(gate_part) * up_part).astype(jnp.bfloat16)

        def add_block(running, block_index):
            hidden_block = lax.dynamic_slice_in_dim(hidden, block_index * block_units, block_units, 1)
            down_block = lax.dynamic_slice_in_dim(down_w, block_index * block_units, block_units, 1)
            partial_value = jnp.dot(hidden_block, down_block.T, preferred_element_type=jnp.float32).astype(jnp.bfloat16)
            partial_value = lax.optimization_barrier(partial_value)
            return (running + partial_value.astype(jnp.float32), None)
        summed, _ = lax.scan(add_block, jnp.zeros((CAP, D), jnp.float32), jnp.arange(N_TP, dtype=jnp.int32))
        expert_out = summed.astype(jnp.bfloat16)
        contribution = weights[:, None] * expert_out.astype(jnp.float32)
        return (accumulated.at[picked].add(contribution), None)
    mixed_out, _ = lax.scan(per_expert, jnp.zeros((TOKENS, D), jnp.float32), (chosen, slot_weight, gate_weight, up_weight, down_weight))
    return mixed_out.astype(jnp.bfloat16)
```

```python
import jax
import jax.numpy as jnp
from jax import lax
from jax.experimental import pallas as pl
from jax.experimental.pallas import tpu as pltpu
from jax.sharding import PartitionSpec as P

EPSILON = 1e-06
N = 8
TOK = 128
SEATS = 8
SLOTS = 256
ROWS = N * N * SEATS
F32, BF16 = jnp.float32, jnp.bfloat16


def dot(a, b, ca, cb):
    return lax.dot_general(a, b, (((ca,), (cb,)), ((), ())), preferred_element_type=F32)


def kernel(
    tokens, gain, chosen, slotw, wg, wu, wd, out,
    W, OH, OHR, WS, OUT, B, A, X, HID, ACC, QS, Q, S, T, R, U, V,
    z_s, z_r, ring_s, ring_r, ry_s, ry_r, rz_s, rz_r, xg_s, xg_r, dg_s, dg_r,
    q_s, q_r, t_s, t_r, u_s, u_r, v_s, v_r,
):
    me = lax.axis_index("ep")
    tp = lax.axis_index("tp")
    z, y = me // N, me % N
    x, c = tp // 2, tp % 2
    weights = (wg, wu, wd)

    def z_peer(d):
        return {"ep": (z + d) % N * N + y}

    def y_peer(d):
        return {"ep": z * N + (y + d) % N}

    def x_peer(d):
        return {"tp": (x + d) % N * 2 + c}

    partner = {"tp": x * 2 + 1 - c}

    def remote(src, dst, send, recv, device):
        return pltpu.make_async_remote_copy(
            src_ref=src, dst_ref=dst, send_sem=send, recv_sem=recv, device_id=device,
            device_id_type=pl.DeviceIdType.MESH,
        )

    def each(count, body):
        def step(i, carry):
            body(i)
            return carry

        lax.fori_loop(0, count, step, 0)

    barrier = pltpu.get_barrier_semaphore()

    def greet(i):
        for peer in (z_peer, y_peer, x_peer):
            pl.semaphore_signal(barrier, inc=1, device_id=peer(i + 1), device_id_type=pl.DeviceIdType.MESH)

    each(N - 1, greet)
    pl.semaphore_signal(barrier, inc=1, device_id=partner, device_id_type=pl.DeviceIdType.MESH)

    for k in range(3):
        W[k, z, y] = weights[k][z]

    tok = chosen[...]
    local = (tok - me * TOK).astype(F32)
    mine = (local >= 0) & (local < TOK)
    first = jnp.sum(jnp.where(local < 0, 1.0, 0.0), axis=1, keepdims=True)
    slot_range = lax.broadcasted_iota(jnp.int32, (N * N, SLOTS), 1).astype(F32)
    key = jnp.where(mine, slot_range - first, -1.0)
    seat = lax.broadcasted_iota(jnp.int32, (N * N, SEATS, SLOTS), 1).astype(F32)
    match = key[:, None, :] == seat
    found = jnp.sum(jnp.where(match, local[:, None, :] + 1.0, 0.0), axis=2, keepdims=True)
    weight = jnp.sum(jnp.where(match, slotw[...][:, None, :], 0.0), axis=2, keepdims=True)
    found = found.reshape(ROWS, 1)
    token_range = lax.broadcasted_iota(jnp.int32, (ROWS, TOK), 1).astype(F32) + 1.0
    pick = jnp.where(found == token_range, 1.0, 0.0).astype(BF16)
    OH[...] = pick
    WS[...] = jnp.broadcast_to(weight.reshape(ROWS, 1), (ROWS, 128))

    values = tokens[...].astype(F32)
    scale = lax.rsqrt(jnp.mean(values * values, axis=1, keepdims=True) + EPSILON)
    columns = pl.ds(pl.multiple_of(tp * 128, 128), 128)
    normed = (tokens[:, columns].astype(F32) * scale * gain[pl.ds(tp, 1), :]).astype(BF16)
    OUT[...] = dot(pick, normed, 1, 0).reshape(N, N, SEATS, 128).astype(BF16)

    owner = (chosen[pl.ds(me, 1), :] // TOK).astype(F32)
    owner_range = lax.broadcasted_iota(jnp.int32, (N * N, SLOTS), 0).astype(F32)
    below = jnp.sum(jnp.where(owner < owner_range, 1.0, 0.0), axis=1, keepdims=True)
    count = jnp.sum(jnp.where(owner == owner_range, 1.0, 0.0), axis=1, keepdims=True)
    seat_of = slot_range - below
    seat_of = jnp.where((seat_of >= 0) & (seat_of < count), seat_of, -1.0)
    OHR[...] = jnp.where(seat_of[:, None, :] == seat, 1.0, 0.0).reshape(ROWS, SLOTS).astype(BF16)

    pl.semaphore_wait(barrier, 3 * (N - 1) + 1)

    def ry(d):
        return remote(OUT.at[:, (y + d) % N], B.at[y], ry_s.at[d - 1], ry_r.at[d - 1], y_peer(d))

    def ry_in(d):
        return remote(OUT.at[:, y], B.at[(y - d) % N], ry_s.at[d - 1], ry_r.at[d - 1], y_peer(d))

    each(N - 1, lambda i: ry(i + 1).start())
    B[y] = OUT[:, y]

    def send_z(k):
        each(
            N - 1,
            lambda i: remote(
                weights[k].at[(z + i + 1) % N], W.at[k, z, y], z_s.at[k, i], z_r.at[k, i], z_peer(i + 1)
            ).start(),
        )

    def wait_z(k, half):
        for i in range(N // 2):
            source = half * (N // 2) + i

            @pl.when(source != z)
            def _():
                d = (z - source) % N
                remote(
                    W.at[k, source, y], W.at[k, source, y], z_s.at[k, d - 1], z_r.at[k, d - 1], z_peer(d)
                ).wait_recv()

    def hops(way, half):
        return 4 if way == half else 3

    def ring(k, half, way, hop):
        sign = 1 - 2 * way
        block = W.at[k, pl.ds(half * 4, 4), (y - sign * hop) % N]
        chunk = k * 2 + half
        return remote(block, block, ring_s.at[way, chunk, hop], ring_r.at[way, chunk, hop], y_peer(sign))

    def ring_in(k, half, way, hop):
        sign = 1 - 2 * way
        block = W.at[k, pl.ds(half * 4, 4), (y - sign * (hop + 1)) % N]
        chunk = k * 2 + half
        return remote(block, block, ring_s.at[way, chunk, hop], ring_r.at[way, chunk, hop], y_peer(sign))

    def ring_hop(kinds, hop):
        for k in kinds:
            for half in range(2):
                if hop == 0:
                    wait_z(k, half)
                for way in range(2):
                    if 0 < hop <= hops(way, half):
                        ring_in(k, half, way, hop - 1).wait_recv()
                    if hop < hops(way, half):
                        ring(k, half, way, hop).start()

    send_z(0)
    send_z(1)

    each(N - 1, lambda i: ry_in(i + 1).wait_recv())

    def rz(d):
        return remote(B.at[:, (z + d) % N], A.at[z], rz_s.at[d - 1], rz_r.at[d - 1], z_peer(d))

    def rz_in(d):
        return remote(B.at[:, z], A.at[(z - d) % N], rz_s.at[d - 1], rz_r.at[d - 1], z_peer(d))

    each(N - 1, lambda i: rz(i + 1).start())
    A[z] = B[:, z]
    send_z(2)

    ring_hop((0, 1), 0)

    each(N - 1, lambda i: rz_in(i + 1).wait_recv())
    arrived = A[...].astype(F32).reshape(ROWS, 128).astype(BF16)
    own_columns = pl.ds(pl.multiple_of(c * 128, 128), 128)
    X[x, :, own_columns] = dot(OHR[...], arrived, 0, 0).astype(BF16)

    def xg(d):
        block = X.at[x, :, own_columns]
        return remote(block, block, xg_s.at[d - 1], xg_r.at[d - 1], x_peer(d))

    def xg_in(d):
        block = X.at[(x - d) % N, :, own_columns]
        return remote(block, block, xg_s.at[d - 1], xg_r.at[d - 1], x_peer(d))

    def dg(d):
        block = X.at[(x - d) % N, :, own_columns]
        return remote(block, block, dg_s.at[d], dg_r.at[d], partner)

    def dg_in(d):
        block = X.at[(x - d) % N, :, pl.ds(pl.multiple_of((1 - c) * 128, 128), 128)]
        return remote(block, block, dg_s.at[d], dg_r.at[d], partner)

    for d in (4, 3, 5, 2, 6, 1, 7):
        xg(d).start()
    dg(0).start()

    ring_hop((0, 1), 1)
    ring_hop((0, 1), 2)
    for d in (1, 7, 2, 6, 3, 5, 4):
        xg_in(d).wait_recv()
        dg(d).start()
    ring_hop((0, 1), 3)
    ring_hop((2,), 0)
    ring_hop((0, 1), 4)
    each(N, lambda d: dg_in(d).wait_recv())

    gate = jnp.zeros((SLOTS, 256), F32)
    up = jnp.zeros((SLOTS, 256), F32)
    for block in range(N):
        rows = X[block]
        gate += dot(rows, W[0, block].reshape(256, 256), 1, 0)
        up += dot(rows, W[1, block].reshape(256, 256), 1, 0)
    HID[...] = (gate / (1.0 + jnp.exp(-gate)) * up).astype(BF16)

    def q_copy(j):
        return remote(QS.at[j], Q.at[j], q_s.at[j], q_r.at[j], partner)

    def t_copy(j, d):
        return remote(S.at[j, (x + d) % N], T.at[x, j], t_s.at[j, d - 1], t_r.at[j, d - 1], x_peer(d))

    def t_in(j, d):
        return remote(S.at[j, x], T.at[(x - d) % N, j], t_s.at[j, d - 1], t_r.at[j, d - 1], x_peer(d))

    def share(b):
        part = dot(W[2, :, b].reshape(256, 256), HID[...], 1, 1)
        j = b % 4

        @pl.when(b // 4 == c)
        def _():
            ACC[j] = part

        @pl.when(b // 4 != c)
        def _():
            QS[j] = part.astype(BF16)
            q_copy(j).start()

    def spread(b):
        j = b % 4

        @pl.when(b // 4 == c)
        def _():
            q_copy(j).wait_recv()
            S[j] = (ACC[j] + Q[j].astype(F32)).reshape(N, 32, SLOTS).astype(BF16)
            T[x, j] = S[j, x]
            for d in (4, 3, 5, 2, 6, 1, 7):
                t_copy(j, d).start()

    share(y)
    for hop in range(1, 5):
        ring_hop((2,), hop)
        if hop < 4:
            share((y - hop) % N)
            spread((y + hop - 1) % N)
            share((y + hop) % N)
            spread((y - hop) % N)
        else:
            share((y + 4) % N)
            spread((y + 3) % N)
            spread((y + 4) % N)

    each(4, lambda j: each(N - 1, lambda i: t_in(j, i + 1).wait_recv()))
    total = T[0].astype(F32)
    for source in range(1, N):
        total += T[source].astype(F32)
    total = total.reshape(128, SLOTS).astype(BF16)

    R[...] = dot(OHR[...], total, 1, 1).reshape(N, N, SEATS, 128).astype(BF16)

    def back_z(d):
        return remote(R.at[(z + d) % N], U.at[z], u_s.at[d - 1], u_r.at[d - 1], z_peer(d))

    def back_z_in(d):
        return remote(R.at[z], U.at[(z - d) % N], u_s.at[d - 1], u_r.at[d - 1], z_peer(d))

    def back_y(d):
        return remote(U.at[:, (y + d) % N], V.at[:, y], v_s.at[d - 1], v_r.at[d - 1], y_peer(d))

    def back_y_in(d):
        return remote(U.at[:, y], V.at[:, (y - d) % N], v_s.at[d - 1], v_r.at[d - 1], y_peer(d))

    each(N - 1, lambda i: back_z(i + 1).start())
    U[z] = R[z]
    each(N - 1, lambda i: back_z_in(i + 1).wait_recv())
    each(N - 1, lambda i: back_y(i + 1).start())
    V[:, y] = U[:, y]
    each(N - 1, lambda i: back_y_in(i + 1).wait_recv())

    weighted = V[...].astype(F32).reshape(ROWS, 128) * WS[...]
    high = weighted.astype(BF16)
    low = (weighted - high.astype(F32)).astype(BF16)
    out[...] = (dot(OH[...], high, 0, 0) + dot(OH[...], low, 0, 0)).astype(BF16)

    def z_sent(i):
        for k in range(3):
            remote(W.at[k, z, y], W.at[k, z, y], z_s.at[k, i], z_r.at[k, i], z_peer(i + 1)).wait_send()
        ry(i + 1).wait_send()
        rz(i + 1).wait_send()
        xg(i + 1).wait_send()
        for j in range(4):
            t_copy(j, i + 1).wait_send()
        back_z(i + 1).wait_send()
        back_y(i + 1).wait_send()

    each(N - 1, z_sent)
    each(N, lambda d: dg(d).wait_send())
    each(4, lambda j: q_copy(j).wait_send())

    def ring_sent(k):
        for half in range(2):
            for way in range(2):
                for hop in range(hops(way, half)):
                    ring(k, half, way, hop).wait_send()

    each(3, ring_sent)


def body(tokens, norm_gain, chosen, slot_weight, gate_weight, up_weight, down_weight):
    dma = pltpu.SemaphoreType.DMA
    vmem = pl.BlockSpec(memory_space=pltpu.VMEM)
    seats = (N, N, SEATS, 128)

    def pair(*shape):
        return [dma(shape), dma(shape)]

    return pl.pallas_call(
        kernel,
        out_shape=jax.ShapeDtypeStruct((TOK, 128), BF16),
        in_specs=[vmem] * 7,
        out_specs=vmem,
        scratch_shapes=[
            pltpu.VMEM((3, N, N, 32, 256), BF16),
            pltpu.VMEM((ROWS, TOK), BF16),
            pltpu.VMEM((ROWS, SLOTS), BF16),
            pltpu.VMEM((ROWS, 128), F32),
            pltpu.VMEM(seats, BF16),
            pltpu.VMEM(seats, BF16),
            pltpu.VMEM(seats, BF16),
            pltpu.VMEM((N, SLOTS, 256), BF16),
            pltpu.VMEM((SLOTS, 256), BF16),
            pltpu.VMEM((4, 256, SLOTS), F32),
            pltpu.VMEM((4, 256, SLOTS), BF16),
            pltpu.VMEM((4, 256, SLOTS), BF16),
            pltpu.VMEM((4, N, 32, SLOTS), BF16),
            pltpu.VMEM((N, 4, 32, SLOTS), BF16),
            pltpu.VMEM(seats, BF16),
            pltpu.VMEM(seats, BF16),
            pltpu.VMEM(seats, BF16),
            *pair(3, N - 1),
            *pair(2, 6, 4),
            *pair(N - 1),
            *pair(N - 1),
            *pair(N - 1),
            *pair(N),
            *pair(4),
            *pair(4, N - 1),
            *pair(N - 1),
            *pair(N - 1),
        ],
        compiler_params=pltpu.CompilerParams(
            collective_id=0, has_side_effects=True, vmem_limit_bytes=40 * 1024 * 1024
        ),
    )(
        tokens,
        norm_gain.reshape(16, 128),
        chosen.reshape(N * N, SLOTS),
        slot_weight.reshape(N * N, SLOTS),
        gate_weight,
        up_weight,
        down_weight,
    )


def solution(mesh):
    in_specs = (
        P("ep", None),
        P(),
        P(),
        P(),
        P(None, "ep", "tp"),
        P(None, "ep", "tp"),
        P(None, "ep", "tp"),
    )
    return jax.shard_map(body, mesh=mesh, in_specs=in_specs, out_specs=P("ep", "tp"), check_vma=False)
```

```python
import jax
import jax.numpy as jnp
from jax import lax
from jax.experimental import pallas as pl
from jax.experimental.pallas import tpu as pltpu
from jax.sharding import PartitionSpec as P

EPSILON = 1e-06
N = 8
TOK = 128
SEATS = 8
SLOTS = 256
ROWS = N * N * SEATS
F32, BF16 = jnp.float32, jnp.bfloat16


def dot(a, b, ca, cb):
    return lax.dot_general(a, b, (((ca,), (cb,)), ((), ())), preferred_element_type=F32)


NEAR = (0, 1, 7, 2, 6, 3, 5, 4)
FAR = (4, 3, 5, 2, 6, 1, 7)


def kernel(
    tokens, gain, chosen, slotw, wg, wu, wd, out,
    TK, GN, CH, SW, SGU, SD, WGU, WD, OH, OHR, WS, OUT, B, B2, A, X, HID, ACC, QS, Q, S, T, R, U, U2, V,
    in_sem, z_s, z_r, zd_s, zd_r, g_s, g_r, d_s, d_r, ry_s, ry_r, rz_s, rz_r, xg_s, xg_r, dg_s, dg_r,
    q_s, q_r, t_s, t_r, u_s, u_r, v_s, v_r,
):
    me = lax.axis_index("ep")
    tp = lax.axis_index("tp")
    z, y = me // N, me % N
    x, c = tp // 2, tp % 2

    def z_peer(d):
        return {"ep": (z + d) % N * N + y}

    def y_peer(d):
        return {"ep": z * N + (y + d) % N}

    def x_peer(d):
        return {"tp": (x + d) % N * 2 + c}

    partner = {"tp": x * 2 + 1 - c}

    def remote(src, dst, send, recv, device):
        return pltpu.make_async_remote_copy(
            src_ref=src, dst_ref=dst, send_sem=send, recv_sem=recv, device_id=device,
            device_id_type=pl.DeviceIdType.MESH,
        )

    def each(count, body):
        def step(i, carry):
            body(i)
            return carry

        lax.fori_loop(0, count, step, 0)

    fetches = [
        pltpu.make_async_copy(source, target, in_sem.at[i])
        for i, (source, target) in enumerate(
            (
                (chosen, CH), (tokens, TK), (slotw, SW), (gain, GN),
                (wg, SGU.at[:, 0]), (wu, SGU.at[:, 1]),
                (wg.at[z], WGU.at[z, y, 0]), (wu.at[z], WGU.at[z, y, 1]),
                (wd, SD), (wd.at[z], WD.at[y, z]),
            )
        )
    ]
    for fetch in fetches:
        fetch.start()

    barrier = pltpu.get_barrier_semaphore()

    def greet(i):
        for peer in (z_peer, y_peer, x_peer):
            pl.semaphore_signal(barrier, inc=1, device_id=peer(i + 1), device_id_type=pl.DeviceIdType.MESH)

    each(N - 1, greet)
    pl.semaphore_signal(barrier, inc=1, device_id=partner, device_id_type=pl.DeviceIdType.MESH)
    for fetch in fetches:
        fetch.wait()

    def pieces(ref):
        return jnp.concatenate([ref[:, i * SLOTS : (i + 1) * SLOTS] for i in range(N)], axis=0)

    local = (pieces(CH) - me * TOK).astype(F32)
    mine = (local >= 0) & (local < TOK)
    first = jnp.sum(jnp.where(local < 0, 1.0, 0.0), axis=1, keepdims=True)
    slot_range = lax.broadcasted_iota(jnp.int32, (N * N, SLOTS), 1).astype(F32)
    key = jnp.where(mine, slot_range - first, -1.0)
    seat = lax.broadcasted_iota(jnp.int32, (N * N, SEATS, SLOTS), 1).astype(F32)
    match = key[:, None, :] == seat
    found = jnp.sum(jnp.where(match, local[:, None, :] + 1.0, 0.0), axis=2, keepdims=True)
    weight = jnp.sum(jnp.where(match, pieces(SW)[:, None, :], 0.0), axis=2, keepdims=True)
    found = found.reshape(ROWS, 1)
    token_range = lax.broadcasted_iota(jnp.int32, (ROWS, TOK), 1).astype(F32) + 1.0
    pick = jnp.where(found == token_range, 1.0, 0.0).astype(BF16)
    OH[...] = pick
    WS[...] = jnp.broadcast_to(weight.reshape(ROWS, 1), (ROWS, 128))

    values = TK[...].astype(F32)
    scale = lax.rsqrt(jnp.mean(values * values, axis=1, keepdims=True) + EPSILON)
    columns = pl.ds(pl.multiple_of(tp * 128, 128), 128)
    normed = (TK[:, columns].astype(F32) * scale * GN[pl.ds(tp, 1), :]).astype(BF16)
    OUT[...] = dot(pick, normed, 1, 0).reshape(N, N, SEATS, 128).astype(BF16)

    owner = (CH[pl.ds(z, 1), pl.ds(pl.multiple_of(y * SLOTS, SLOTS), SLOTS)] // TOK).astype(F32)
    owner_range = lax.broadcasted_iota(jnp.int32, (N * N, SLOTS), 0).astype(F32)
    below = jnp.sum(jnp.where(owner < owner_range, 1.0, 0.0), axis=1, keepdims=True)
    count = jnp.sum(jnp.where(owner == owner_range, 1.0, 0.0), axis=1, keepdims=True)
    seat_of = slot_range - below
    seat_of = jnp.where((seat_of >= 0) & (seat_of < count), seat_of, -1.0)
    OHR[...] = jnp.where(seat_of[:, None, :] == seat, 1.0, 0.0).reshape(ROWS, SLOTS).astype(BF16)

    pl.semaphore_wait(barrier, 3 * (N - 1) + 1)

    def ry(d):
        return remote(OUT.at[(y + d) % N], B.at[y], ry_s.at[d - 1], ry_r.at[d - 1], y_peer(d))

    def ry_in(d):
        return remote(OUT.at[y], B.at[(y - d) % N], ry_s.at[d - 1], ry_r.at[d - 1], y_peer(d))

    def rz(d):
        return remote(B2.at[(z + d) % N], A.at[z], rz_s.at[d - 1], rz_r.at[d - 1], z_peer(d))

    def rz_in(d):
        return remote(B2.at[z], A.at[(z - d) % N], rz_s.at[d - 1], rz_r.at[d - 1], z_peer(d))

    def zgu(d):
        return remote(SGU.at[(z + d) % N], WGU.at[z, y], z_s.at[d - 1], z_r.at[d - 1], z_peer(d))

    def zgu_in(d):
        return remote(SGU.at[z], WGU.at[(z - d) % N, y], z_s.at[d - 1], z_r.at[d - 1], z_peer(d))

    def zd(d):
        return remote(SD.at[(z + d) % N], WD.at[y, z], zd_s.at[d - 1], zd_r.at[d - 1], z_peer(d))

    def zd_in(d):
        return remote(SD.at[z], WD.at[y, (z - d) % N], zd_s.at[d - 1], zd_r.at[d - 1], z_peer(d))

    def hops(way, chunk):
        return 4 if way == chunk % 2 else 3

    def gu(chunk, way, hop, come):
        sign = 1 - 2 * way
        block = WGU.at[(z + NEAR[chunk]) % N, (y - sign * (hop + come)) % N]
        return remote(block, block, g_s.at[way, chunk, hop], g_r.at[way, chunk, hop], y_peer(sign))

    def down(chunk, way, hop, come):
        sign = 1 - 2 * way
        block = WD.at[(y - sign * (hop + come)) % N, pl.ds(chunk * 2, 2)]
        return remote(block, block, d_s.at[way, chunk, hop], d_r.at[way, chunk, hop], y_peer(sign))

    def ring(copy, chunk, hop):
        for way in range(2):
            if 0 < hop <= hops(way, chunk):
                copy(chunk, way, hop - 1, 1).wait_recv()
            if hop < hops(way, chunk):
                copy(chunk, way, hop, 0).start()

    def gu_first(chunk):
        if chunk > 0:
            zgu_in((N - NEAR[chunk]) % N).wait_recv()
        ring(gu, chunk, 0)

    each(N - 1, lambda i: ry(i + 1).start())
    for d in NEAR[1:]:
        zgu(d).start()
    B[y] = OUT[y]
    for chunk in range(5):
        gu_first(chunk)

    each(N - 1, lambda i: ry_in(i + 1).wait_recv())
    for i in range(N):
        B2[i] = B[:, i]
    each(N - 1, lambda i: rz(i + 1).start())
    for d in NEAR[1:]:
        zd(d).start()
    A[z] = B2[z]

    ring(gu, 0, 1)
    gu_first(5)
    gu_first(6)
    ring(gu, 1, 1)
    gu_first(7)
    for chunk in (2, 3, 4):
        ring(gu, chunk, 1)

    each(N - 1, lambda i: rz_in(i + 1).wait_recv())
    arrived = A[...].astype(F32).reshape(ROWS, 128).astype(BF16)
    own_columns = pl.ds(pl.multiple_of(c * 128, 128), 128)
    X[x, :, own_columns] = dot(OHR[...], arrived, 0, 0).astype(BF16)

    def xg(d):
        block = X.at[x, :, own_columns]
        return remote(block, block, xg_s.at[d - 1], xg_r.at[d - 1], x_peer(d))

    def xg_in(d):
        block = X.at[(x - d) % N, :, own_columns]
        return remote(block, block, xg_s.at[d - 1], xg_r.at[d - 1], x_peer(d))

    def dg(d):
        block = X.at[(x - d) % N, :, own_columns]
        return remote(block, block, dg_s.at[d], dg_r.at[d], partner)

    def dg_in(d):
        block = X.at[(x - d) % N, :, pl.ds(pl.multiple_of((1 - c) * 128, 128), 128)]
        return remote(block, block, dg_s.at[d], dg_r.at[d], partner)

    for d in FAR:
        xg(d).start()
    dg(0).start()

    for chunk in (5, 6, 7):
        ring(gu, chunk, 1)
    for hop in (2, 3):
        for chunk in range(8):
            ring(gu, chunk, hop)
    each(N - 1, lambda i: zd_in(i + 1).wait_recv())
    for chunk in range(4):
        ring(down, chunk, 0)
    for d in (1, 7, 2, 6, 3, 5, 4):
        xg_in(d).wait_recv()
        dg(d).start()
    for chunk in range(8):
        ring(gu, chunk, 4)
    each(N, lambda d: dg_in(d).wait_recv())

    gate = jnp.zeros((SLOTS, 256), F32)
    up = jnp.zeros((SLOTS, 256), F32)
    for block in range(N):
        rows = X[block]
        gate += dot(rows, WGU[block, :, 0].reshape(256, 256), 1, 0)
        up += dot(rows, WGU[block, :, 1].reshape(256, 256), 1, 0)
    HID[...] = (gate / (1.0 + jnp.exp(-gate)) * up).astype(BF16)

    def q_copy(j):
        return remote(QS.at[j], Q.at[j], q_s.at[j], q_r.at[j], partner)

    def t_copy(j, d):
        return remote(S.at[j, (x + d) % N], T.at[x, j], t_s.at[j, d - 1], t_r.at[j, d - 1], x_peer(d))

    def t_in(j, d):
        return remote(S.at[j, x], T.at[(x - d) % N, j], t_s.at[j, d - 1], t_r.at[j, d - 1], x_peer(d))

    def share(b):
        part = dot(WD[b].reshape(256, 256), HID[...], 1, 1)
        j = b % 4

        @pl.when(b // 4 == c)
        def _():
            ACC[j] = part

        @pl.when(b // 4 != c)
        def _():
            QS[j] = part.astype(BF16)
            q_copy(j).start()

    def spread(b):
        j = b % 4

        @pl.when(b // 4 == c)
        def _():
            q_copy(j).wait_recv()
            S[j] = (ACC[j] + Q[j].astype(F32)).reshape(N, 32, SLOTS).astype(BF16)
            T[x, j] = S[j, x]
            for d in FAR:
                t_copy(j, d).start()

    share(y)
    for hop in range(1, 5):
        for chunk in range(4):
            ring(down, chunk, hop)
        if hop < 4:
            share((y - hop) % N)
            spread((y + hop - 1) % N)
            share((y + hop) % N)
            spread((y - hop) % N)
        else:
            share((y + 4) % N)
            spread((y + 3) % N)
            spread((y + 4) % N)

    each(4, lambda j: each(N - 1, lambda i: t_in(j, i + 1).wait_recv()))
    total = T[0].astype(F32)
    for source in range(1, N):
        total += T[source].astype(F32)
    total = total.reshape(128, SLOTS).astype(BF16)

    R[...] = dot(OHR[...], total, 1, 1).reshape(N, N, SEATS, 128).astype(BF16)

    def back_z(d):
        return remote(R.at[(z + d) % N], U.at[z], u_s.at[d - 1], u_r.at[d - 1], z_peer(d))

    def back_z_in(d):
        return remote(R.at[z], U.at[(z - d) % N], u_s.at[d - 1], u_r.at[d - 1], z_peer(d))

    def back_y(d):
        return remote(U2.at[(y + d) % N], V.at[y], v_s.at[d - 1], v_r.at[d - 1], y_peer(d))

    def back_y_in(d):
        return remote(U2.at[y], V.at[(y - d) % N], v_s.at[d - 1], v_r.at[d - 1], y_peer(d))

    for d in FAR:
        back_z(d).start()
    U[z] = R[z]
    each(N - 1, lambda i: back_z_in(i + 1).wait_recv())
    for i in range(N):
        U2[i] = U[:, i]
    for d in FAR:
        back_y(d).start()
    V[y] = U2[y]
    each(N - 1, lambda i: back_y_in(i + 1).wait_recv())

    weighted = V[...].astype(F32).reshape(ROWS, 128) * WS[...]
    high = weighted.astype(BF16)
    low = (weighted - high.astype(F32)).astype(BF16)
    out[...] = (dot(OH[...], high, 0, 0) + dot(OH[...], low, 0, 0)).astype(BF16)

    def sent(i):
        for copy in (ry, rz, zgu, zd, xg, back_z, back_y):
            copy(i + 1).wait_send()
        for j in range(4):
            t_copy(j, i + 1).wait_send()

    each(N - 1, sent)
    each(N, lambda d: dg(d).wait_send())
    each(4, lambda j: q_copy(j).wait_send())
    for copy, count in ((gu, 8), (down, 4)):
        for chunk in range(count):
            for way in range(2):
                for hop in range(hops(way, chunk)):
                    copy(chunk, way, hop, 0).wait_send()


def body(tokens, norm_gain, chosen, slot_weight, gate_weight, up_weight, down_weight):
    dma = pltpu.SemaphoreType.DMA
    seats = pltpu.VMEM((N, N, SEATS, 128), BF16)

    def pair(*shape):
        return [dma(shape), dma(shape)]

    return pl.pallas_call(
        kernel,
        out_shape=jax.ShapeDtypeStruct((TOK, 128), BF16),
        in_specs=[pl.BlockSpec(memory_space=pl.ANY)] * 7,
        out_specs=pl.BlockSpec(memory_space=pltpu.VMEM),
        scratch_shapes=[
            pltpu.VMEM((TOK, 2048), BF16),
            pltpu.VMEM((16, 128), F32),
            pltpu.VMEM((N, N * SLOTS), jnp.int32),
            pltpu.VMEM((N, N * SLOTS), F32),
            pltpu.VMEM((N, 2, 32, 256), BF16),
            pltpu.VMEM((N, 32, 256), BF16),
            pltpu.VMEM((N, N, 2, 32, 256), BF16),
            pltpu.VMEM((N, N, 32, 256), BF16),
            pltpu.VMEM((ROWS, TOK), BF16),
            pltpu.VMEM((ROWS, SLOTS), BF16),
            pltpu.VMEM((ROWS, 128), F32),
            *[seats] * 4,
            pltpu.VMEM((N, SLOTS, 256), BF16),
            pltpu.VMEM((SLOTS, 256), BF16),
            pltpu.VMEM((4, 256, SLOTS), F32),
            pltpu.VMEM((4, 256, SLOTS), BF16),
            pltpu.VMEM((4, 256, SLOTS), BF16),
            pltpu.VMEM((4, N, 32, SLOTS), BF16),
            pltpu.VMEM((N, 4, 32, SLOTS), BF16),
            *[seats] * 4,
            dma((10,)),
            *pair(N - 1),
            *pair(N - 1),
            *pair(2, 8, 4),
            *pair(2, 4, 4),
            *pair(N - 1),
            *pair(N - 1),
            *pair(N - 1),
            *pair(N),
            *pair(4),
            *pair(4, N - 1),
            *pair(N - 1),
            *pair(N - 1),
        ],
        compiler_params=pltpu.CompilerParams(
            collective_id=0, has_side_effects=True, vmem_limit_bytes=60 * 1024 * 1024
        ),
    )(tokens, norm_gain.reshape(16, 128), chosen, slot_weight, gate_weight, up_weight, down_weight)


def solution(mesh):
    in_specs = (
        P("ep", None),
        P(),
        P(),
        P(),
        P(None, "ep", "tp"),
        P(None, "ep", "tp"),
        P(None, "ep", "tp"),
    )
    return jax.shard_map(body, mesh=mesh, in_specs=in_specs, out_specs=P("ep", "tp"), check_vma=False)
```
